32 devices in a mesh: sp: 16 (over z, y, x), tp: 2 (over core).
Axes of the slice: x: 2, y: 2, z: 4, core: 2. Of those that a mesh axis runs over, the one named last changes fastest.
Arguments:
- resid: bfloat16 [4096, 2048], P(('sp', 'tp')), may hold values from -3 to 3
- queries: bfloat16 [4096, 1024], P('sp', 'tp'), may hold values from -8 to 8
- keys: bfloat16 [4096, 256], P('sp', 'tp'), may hold values from -8 to 8
- values: bfloat16 [4096, 256], P('sp', 'tp'), may hold values from -6 to 6
- docs: int32 [4096], P('sp'), may hold values from 0 to 3, never falling along the last dimension, each value on 1 to 2048 neighbouring positions
- sink: float32 [8], P('tp'), may hold values from 2 to 6
- w_out: bfloat16 [1024, 2048], replicated, may hold values from -0.375 to 0.375
- norm_gain: float32 [2048], replicated, may hold values from 0.1 to 1.9
- w_gate: bfloat16 [16, 2048, 1024], P('sp', None, 'tp'), may hold values from -0.125 to 0.125
- w_up: bfloat16 [16, 2048, 1024], P('sp', None, 'tp'), may hold values from -0.125 to 0.125
- w_down: bfloat16 [16, 1024, 2048], P('sp', 'tp'), may hold values from -0.1875 to 0.1875
- expert_ids: int32 [4096, 2], P(('sp', 'tp')), may hold values from 0 to 15, all different within a row; in each aligned block of 128 rows (0 to 127, 128 to 255, ...) at most 32 rows name the same one
- route_weights: float32 [4096, 2], P(('sp', 'tp')), may hold values from 0.1 to 0.9
Outputs:
- layer_out: bfloat16 [4096, 2048], P(('sp', 'tp'))
The draws below stay inside these ranges and needn't reach their ends.
Inputs may be any that keep to these rules, and one draw needn't show every extreme that they name: `docs`: document numbers never fall along the sequence; a document holds at most 2048 positions. `expert_ids`: each row names 2 different experts. The rows of one device (aligned blocks of 256 // 2 rows) name one expert at most 32 times, and in every draw some expert is named exactly 32 times by some device.
All inputs are finite; a program needn't handle non-finite values.
Results may differ from the reference program's by a relative error of at most 0.007.
Values may be sent and summed in bfloat16 or wider, within the bound.
A program may use at most 128 MiB of HBM per device.

```python
import math
import jax
import jax.numpy as jnp
import numpy as np
from jax import lax

D = 2048
QUERY_HEADS = 8
KEY_VALUE_HEADS = 2
HEAD_WIDTH = 128
WINDOW_RADIUS = 128
FF = 1024
TOP_K = 2
TOK_DEV = 256
SEQUENCE_TOKENS = 4096
EXPERTS = 16
CAP = 32
DOCS = 4
LONGEST = 2048
N_SP = 16
N_TP = 2


def query_key_pair(key):
    base = jax.random.fold_in(key, 7)
    kq, key_window = jax.random.split(base)
    keys = jnp.clip(jax.random.normal(key_window, (SEQUENCE_TOKENS, KEY_VALUE_HEADS * HEAD_WIDTH), jnp.float32), -6.0, 6.0)
    queries = jnp.clip(1.5 * jax.random.normal(kq, (SEQUENCE_TOKENS, QUERY_HEADS * HEAD_WIDTH), jnp.float32), -8.0, 8.0)
    return (queries, keys)


def draw_queries(key, part):
    return query_key_pair(key)[0].astype(jnp.bfloat16)


def draw_keys(key, part):
    return query_key_pair(key)[1].astype(jnp.bfloat16)


def levels(own_key, extent, cuts, low, largest):
    gain, own = 1.0, jax.random.fold_in(own_key, 6)
    for position, shards_of in cuts:
        steps = jnp.exp(jax.random.uniform(jax.random.fold_in(own, position), (shards_of,), jnp.float32, low / len(cuts), largest / len(cuts)))
        gain = gain * jnp.repeat(steps, extent[position] // shards_of).reshape([-1 if axis == position else 1 for axis in range(len(extent))])
    return gain


def split_up(count, total, bound, lean):
    weights = [(1 << 20) // math.isqrt(standing ** lean) + 1 for standing in range(2, count + 1)]
    spare, given = total - bound - (count - 1), [1] * (count - 1)
    while spare > 0:
        candidates = [i for i in range(count - 1) if given[i] < bound]
        pool, budget = sum([weights[i] for i in candidates]), spare
        for i in candidates:
            addition = min(bound - given[i], max(1, budget * weights[i] // pool), spare)
            given[i] = given[i] + addition
            spare = spare - addition
    return np.array([bound] + given)


def uneven(own_key, amount, total, reach, slope):
    if amount == 2:
        one = jax.random.randint(own_key, (), max(1, total - reach), min(reach, total - 1) + 1)
        return jnp.stack([one, total - one])
    tallies = jnp.asarray(split_up(amount, total, reach, slope), jnp.int32)
    pairs = (amount - 1) // 2
    giver, taker = tallies[1:1 + 2 * pairs:2], tallies[2:2 + 2 * pairs:2]
    margin = jnp.minimum(giver - 1, reach - taker)
    shifted = jax.random.randint(jax.random.fold_in(own_key, 1), (pairs,), 0, 1 << 20) % (margin + 1)
    tallies = tallies.at[1:1 + 2 * pairs:2].set(giver - shifted).at[2:2 + 2 * pairs:2].set(taker + shifted)
    return tallies[jax.random.permutation(jax.random.fold_in(own_key, 2), amount)]


def deal_out(key, own, number, rows, number_of, top, reach, slope):
    order = jax.random.permutation(key, number_of)
    crowded, ordinary = load_shares(number_of, rows * top, reach, slope, True), load_shares(number_of, rows * top, reach, slope, False)
    places = jnp.arange(number_of)

    def named(sizes, rotation):
        used = int((sizes > 0).sum())
        fixed = max(1, used // 4)
        passed = fixed + (places - fixed + rotation * (used - fixed)) % max(1, number_of - fixed)
        return jnp.zeros((number_of,), jnp.int32).at[order[jnp.where(places < fixed, places, passed)]].set(jnp.asarray(sizes, jnp.int32))

    sizes = jnp.where(number % 4 == 0, named(crowded, number // 4), named(ordinary, number - number // 4 - 1))
    mixed = jax.random.permutation(jax.random.fold_in(own, 3), number_of)
    source_of, receiver = mixed[0:number_of // 2 * 2:2], mixed[1:number_of // 2 * 2:2]
    margin = jnp.minimum(sizes[source_of] - 1, reach - sizes[receiver]) // 2
    margin = jnp.where((source_of == order[0]) | (receiver == order[0]) | (sizes[receiver] == 0), 0, jnp.maximum(margin, 0))
    passed = jax.random.randint(jax.random.fold_in(own, 4), (number_of // 2,), 0, 1 << 20) % (margin + 1)
    sizes = sizes.at[source_of].add(-passed).at[receiver].add(passed)
    members = jnp.searchsorted(jnp.cumsum(sizes), jnp.arange(rows * top), side="right").astype(jnp.int32)
    grid = members.reshape(top, rows).T
    grid = grid[jax.random.permutation(jax.random.fold_in(own, 1), rows)]
    rotation = jax.random.randint(jax.random.fold_in(own, 2), (rows, 1), 0, top)
    return jnp.take_along_axis(grid, (jnp.arange(top)[None, :] + rotation) % top, axis=1)


def load_shares(amount, total, most, slope, full):
    portions = [(1 << 20) // math.isqrt(grade ** slope) + 1 for grade in range(1, amount + 1)]
    largest = most if full else min(most, max(-(-total // amount), total * portions[0] // sum(portions)))
    least = 1 if total - largest >= amount - 1 else 0
    given, surplus = [largest] + [least] * (amount - 1), total - largest - least * (amount - 1)
    while surplus > 0:
        candidates = [i for i in range(1, amount) if given[i] < largest] or [i for i in range(1, amount) if given[i] < most]
        whole, budget = sum([portions[i] for i in candidates]), surplus
        for i in candidates:
            more = min(most - given[i], max(1, budget * portions[i] // whole), surplus)
            given[i] = given[i] + more
            surplus = surplus - more
    return np.array(given)


def normal_values(stream_key, dims, width, bound, cuts=(), kind=jnp.bfloat16):
    level = levels(stream_key, dims, cuts, -0.22, 0.18) if cuts else 1.0
    drawn = jax.random.normal(stream_key, dims, jnp.float32) * width * level
    return jnp.minimum(jnp.maximum(drawn, -bound), bound).astype(kind)


def setup_inputs(seed: int = 0) -> dict:
    seeds = jax.random.split(jax.random.key(seed), 14)
    resid = normal_values(seeds[0], (SEQUENCE_TOKENS, D), 0.5, 3.0, ((0, 32),))
    queries = draw_queries(jax.random.fold_in(seeds[13], 71), 0)
    keys = draw_keys(jax.random.fold_in(seeds[13], 71), 0)
    values = normal_values(seeds[3], (SEQUENCE_TOKENS, KEY_VALUE_HEADS * HEAD_WIDTH), 1.0, 6.0, ((0, 16), (1, 2)))
    docs = jnp.searchsorted(jnp.cumsum(uneven(seeds[4], DOCS, SEQUENCE_TOKENS, LONGEST, 2)), jnp.arange(SEQUENCE_TOKENS), side="right").astype(jnp.int32)
    sink = jnp.clip(2.0 + 4.0 * jax.random.uniform(seeds[5], (QUERY_HEADS,), jnp.float32) ** levels(seeds[5], (QUERY_HEADS,), ((0, 2),), -0.2, 0.2), 2.0, 6.0)
    w_out = normal_values(seeds[6], (QUERY_HEADS * HEAD_WIDTH, D), (QUERY_HEADS * HEAD_WIDTH // 4) ** -0.5, 0.375)
    norm_gain = jnp.clip(1.0 + 0.18 * jax.random.normal(seeds[7], (D,), jnp.float32), 0.1, 1.9)
    w_gate = normal_values(seeds[8], (EXPERTS, D, FF), D ** -0.5, 0.125, ((0, 16), (2, 2)))
    w_up = normal_values(seeds[9], (EXPERTS, D, FF), D ** -0.5, 0.125, ((0, 16), (2, 2)))
    w_down = normal_values(seeds[10], (EXPERTS, FF, D), FF ** -0.5, 0.1875, ((0, 16), (1, 2)))
    expert_ids_keys = jax.random.split(jax.random.fold_in(seeds[11], 1), SEQUENCE_TOKENS // (TOK_DEV // N_TP))
    expert_ids_turns = jax.random.permutation(jax.random.fold_in(seeds[11], 3), SEQUENCE_TOKENS // (TOK_DEV // N_TP))
    expert_ids = jax.vmap(lambda own, number: deal_out(jax.random.fold_in(seeds[11], 2), own, number, TOK_DEV // N_TP, EXPERTS, TOP_K, CAP, 2))(expert_ids_keys, expert_ids_turns).reshape((SEQUENCE_TOKENS, TOP_K))
    route_weights = jnp.clip(0.1 + 0.79999997 * jax.random.uniform(seeds[12], (SEQUENCE_TOKENS, TOP_K), jnp.float32) ** levels(seeds[12], (SEQUENCE_TOKENS, TOP_K), ((0, 32),), -0.2, 0.2), 0.1, 0.9)
    return dict(resid=resid, queries=queries, keys=keys, values=values, docs=docs, sink=sink, w_out=w_out, norm_gain=norm_gain, w_gate=w_gate, w_up=w_up, w_down=w_down, expert_ids=expert_ids, route_weights=route_weights)


eps = 1e-06

def window_band(table):
    return jnp.concatenate([table[:-2], table[1:-1], table[2:]], axis=1)

def reference(resid, queries, keys, values, docs, sink, w_out, norm_gain, w_gate, w_up, w_down, expert_ids, route_weights):
    query_blocks = SEQUENCE_TOKENS // WINDOW_RADIUS
    head_group = QUERY_HEADS // KEY_VALUE_HEADS
    query_block = queries.astype(jnp.float32).reshape(query_blocks, WINDOW_RADIUS, KEY_VALUE_HEADS, head_group, HEAD_WIDTH)
    padded_keys = jnp.pad(keys.astype(jnp.float32), ((WINDOW_RADIUS, WINDOW_RADIUS), (0, 0))).reshape(query_blocks + 2, WINDOW_RADIUS, KEY_VALUE_HEADS, HEAD_WIDTH)
    padded_values = jnp.pad(values.astype(jnp.float32), ((WINDOW_RADIUS, WINDOW_RADIUS), (0, 0))).reshape(query_blocks + 2, WINDOW_RADIUS, KEY_VALUE_HEADS, HEAD_WIDTH)
    dpad = jnp.pad(docs, (WINDOW_RADIUS, WINDOW_RADIUS), constant_values=-1).reshape(query_blocks + 2, WINDOW_RADIUS)
    kband = window_band(padded_keys)
    value_window = window_band(padded_values)
    dband = window_band(dpad)
    scores = jnp.einsum('nqhgd,nkhd->nhgqk', query_block, kband) * HEAD_WIDTH ** (-0.5)
    qpos = jnp.arange(query_blocks)[:, None] * WINDOW_RADIUS + jnp.arange(WINDOW_RADIUS)[None, :]
    kpos = (jnp.arange(query_blocks)[:, None] - 1) * WINDOW_RADIUS + jnp.arange(3 * WINDOW_RADIUS)[None, :]
    offset = kpos[:, None, :] - qpos[:, :, None]
    qdoc = docs.reshape(query_blocks, WINDOW_RADIUS)
    valid = (jnp.abs(offset) <= WINDOW_RADIUS) & (dband[:, None, :] == qdoc[:, :, None])
    valid = valid[:, None, None]
    sink_logits = sink.astype(jnp.float32).reshape(1, KEY_VALUE_HEADS, head_group, 1, 1)
    top = jnp.maximum(lax.optimization_barrier(jnp.max(jnp.where(valid, scores, -jnp.inf), axis=-1, keepdims=True)), sink_logits)
    expo = jnp.where(valid, jnp.exp(scores - top), 0.0)
    denom = lax.optimization_barrier(jnp.sum(expo, axis=-1, keepdims=True)) + jnp.exp(sink_logits - top)
    probs = lax.optimization_barrier((expo / denom).astype(jnp.bfloat16))
    attended = jnp.einsum('nhgqk,nkhd->nqhgd', probs.astype(jnp.float32), value_window).astype(jnp.bfloat16)
    attended = attended.reshape(SEQUENCE_TOKENS, QUERY_HEADS * HEAD_WIDTH)
    mixed = resid.astype(jnp.float32) + jnp.dot(attended, w_out, preferred_element_type=jnp.float32)
    normed = (mixed * lax.rsqrt(lax.optimization_barrier(jnp.mean(mixed * mixed, axis=-1, keepdims=True)) + eps) * norm_gain.astype(jnp.float32)).astype(jnp.bfloat16)
    visits = SEQUENCE_TOKENS * TOP_K
    most = N_SP * N_TP * CAP
    flat = expert_ids.reshape(visits).astype(jnp.int32)
    order = jnp.argsort(flat, stable=True).astype(jnp.int32)
    sorted_e = flat[order]
    counts = jnp.bincount(flat, length=EXPERTS).astype(jnp.int32)
    starts = (jnp.cumsum(counts) - counts).astype(jnp.int32)
    slot_sorted = sorted_e * most + jnp.arange(visits, dtype=jnp.int32) - starts[sorted_e]
    slot = jnp.zeros((visits,), jnp.int32).at[order].set(slot_sorted.astype(jnp.int32))
    owner = jnp.arange(visits, dtype=jnp.int32) // TOP_K
    table = jnp.zeros((EXPERTS * most, D), jnp.bfloat16).at[slot].set(normed[owner]).reshape(EXPERTS, most, D)

    def run(packed):
        rows, wg, wu, wd = packed
        hidden = (jax.nn.silu(jnp.dot(rows, wg, preferred_element_type=jnp.float32)) * jnp.dot(rows, wu, preferred_element_type=jnp.float32)).astype(jnp.bfloat16)
        part = FF // N_TP
        total = jnp.zeros((most, D), jnp.float32)
        for piece in range(N_TP):
            partial_value = jnp.dot(hidden[:, piece * part:(piece + 1) * part], wd[piece * part:(piece + 1) * part], preferred_element_type=jnp.float32).astype(jnp.bfloat16)
            total = total + partial_value.astype(jnp.float32)
        return total.astype(jnp.bfloat16)
    outs = lax.map(run, (table, w_gate, w_up, w_down)).reshape(EXPERTS * most, D)
    got = outs[slot].astype(jnp.float32).reshape(SEQUENCE_TOKENS, TOP_K, D)
    extra = lax.optimization_barrier(jnp.sum(route_weights.astype(jnp.float32)[:, :, None] * got, axis=1))
    return (mixed + extra).astype(jnp.bfloat16)
```

```python
import functools

import jax
import jax.numpy as jnp
from jax import lax
from jax.experimental import pallas as pl
from jax.experimental.pallas import tpu as pltpu
from jax.sharding import PartitionSpec as P

HEAD_WIDTH = 128
RADIUS = 128
EPS = 1e-06
MESH = pl.DeviceIdType.MESH
F32 = jnp.float32
BF16 = jnp.bfloat16


def kernel(
    n_sp,
    n_tp,
    cap,
    resid_hbm,
    q_ref,
    k_ref,
    v_ref,
    docs_ref,
    sink_ref,
    wout_hbm,
    gain_ref,
    gate_hbm,
    up_hbm,
    down_hbm,
    ids_ref,
    rw_ref,
    out_ref,
    kext,
    vext,
    dext,
    gbuf,
    ubuf,
    dbuf,
    wobuf,
    resid,
    att,
    attsend,
    mixed,
    outgoing,
    landed,
    ret,
    back,
    halo_send,
    halo_recv,
    w_send,
    w_recv,
    loc_sem,
    att_send_sem,
    att_recv_sem,
    d_send,
    d_recv,
    r_send,
    r_recv,
):
    sp = lax.axis_index("sp")
    tp = lax.axis_index("tp")
    other = n_tp - 1 - tp
    rows_all = q_ref.shape[0]
    heads = q_ref.shape[1] // HEAD_WIDTH
    nb = rows_all // RADIUS
    keep = rows_all // n_tp
    width = q_ref.shape[1]
    dim = out_ref.shape[1]
    total_pos = n_sp * rows_all

    barrier = pltpu.get_barrier_semaphore()

    @pl.loop(1, n_sp)
    def _(o):
        pl.semaphore_signal(
            barrier, inc=1, device_id=(lax.rem(sp + o, n_sp), tp), device_id_type=MESH
        )

    pl.semaphore_signal(barrier, inc=1, device_id=(sp, other), device_id_type=MESH)

    local_copies = [
        pltpu.make_async_copy(wout_hbm, wobuf, loc_sem.at[0]),
        pltpu.make_async_copy(resid_hbm, resid, loc_sem.at[1]),
        pltpu.make_async_copy(gate_hbm.at[0], gbuf.at[tp], loc_sem.at[2]),
        pltpu.make_async_copy(up_hbm.at[0], ubuf.at[tp], loc_sem.at[3]),
        pltpu.make_async_copy(down_hbm.at[0], dbuf.at[tp], loc_sem.at[4]),
    ]
    for c in local_copies[:2]:
        c.start()

    pl.semaphore_wait(barrier, n_sp)

    right = (lax.rem(sp + 1, n_sp), tp)
    left = (lax.rem(sp + n_sp - 1, n_sp), tp)
    tail = rows_all - RADIUS
    end = rows_all + RADIUS

    def remote(src, dst, s, r, dev):
        return pltpu.make_async_remote_copy(
            src_ref=src, dst_ref=dst, send_sem=s, recv_sem=r, device_id=dev, device_id_type=MESH
        )

    halo = []
    for i, (src, dst) in enumerate(((k_ref, kext), (v_ref, vext))):
        halo.append(
            remote(
                src.at[pl.ds(tail, RADIUS)],
                dst.at[pl.ds(0, RADIUS)],
                halo_send.at[2 * i],
                halo_recv.at[2 * i],
                right,
            )
        )
        halo.append(
            remote(
                src.at[pl.ds(0, RADIUS)],
                dst.at[pl.ds(end, RADIUS)],
                halo_send.at[2 * i + 1],
                halo_recv.at[2 * i + 1],
                left,
            )
        )
    halo.append(
        remote(docs_ref.at[nb - 1], dext.at[0], halo_send.at[4], halo_recv.at[4], right)
    )
    halo.append(
        remote(docs_ref.at[0], dext.at[nb + 1], halo_send.at[5], halo_recv.at[5], left)
    )
    for c in halo:
        c.start()
    partner = (sp, other)
    weights = [
        remote(gate_hbm.at[0], gbuf.at[tp], w_send.at[0], w_recv.at[0], partner),
        remote(up_hbm.at[0], ubuf.at[tp], w_send.at[1], w_recv.at[1], partner),
        remote(down_hbm.at[0], dbuf.at[tp], w_send.at[2], w_recv.at[2], partner),
    ]
    for c in weights:
        c.start()
    for c in local_copies[2:]:
        c.start()

    kext[RADIUS:end, :] = k_ref[...]
    vext[RADIUS:end, :] = v_ref[...]
    for b in range(nb):
        dext[b + 1] = docs_ref[b]

    me = sp
    top_k = ids_ref.shape[1]
    n_slots = n_sp * cap
    lane = lax.broadcasted_iota(jnp.int32, (keep, n_sp), 1)
    hots = [(ids_ref[:, k : k + 1] == lane).astype(F32) for k in range(top_k)]
    visits = sum(hots)
    lower = (
        lax.broadcasted_iota(jnp.int32, (keep, keep), 1)
        < lax.broadcasted_iota(jnp.int32, (keep, keep), 0)
    ).astype(BF16)
    before = jnp.dot(lower, visits.astype(BF16), preferred_element_type=F32)
    slot_lane = lax.broadcasted_iota(jnp.int32, (keep, n_slots), 1).astype(F32)
    picks = []
    for k in range(top_k):
        rank = jnp.sum(hots[k] * before, axis=1, keepdims=True)
        rel = ids_ref[:, k : k + 1] - me
        rel = jnp.where(rel < 0, rel + n_sp, rel)
        slot = rel.astype(F32) * float(cap) + rank
        picks.append((slot == slot_lane).astype(BF16))

    for c in halo:
        c.wait()

    eye = lax.broadcasted_iota(jnp.int32, (RADIUS, RADIUS), 0) == lax.broadcasted_iota(
        jnp.int32, (RADIUS, RADIUS), 1
    )

    def attend(b):
        row0 = pl.multiple_of(b * RADIUS, RADIUS)
        keys = kext[pl.ds(row0, 3 * RADIUS), :]
        vals = vext[pl.ds(row0, 3 * RADIUS), :]
        kdoc = jnp.concatenate([dext[b], dext[b + 1], dext[b + 2]], axis=1)
        qdoc = jnp.sum(
            jnp.where(eye, jnp.broadcast_to(dext[b + 1], (RADIUS, RADIUS)), 0).astype(F32),
            axis=1,
            keepdims=True,
        )
        qi = lax.broadcasted_iota(jnp.int32, (RADIUS, 3 * RADIUS), 0)
        kj = lax.broadcasted_iota(jnp.int32, (RADIUS, 3 * RADIUS), 1)
        where_key = kj + (sp * rows_all + (b - 1) * RADIUS)
        valid = (
            (kj >= qi)
            & (kj <= qi + 2 * RADIUS)
            & (where_key >= 0)
            & (where_key < total_pos)
            & (kdoc.astype(F32) == qdoc)
        )
        parts = []
        for h in range(heads):
            qh = q_ref[pl.ds(row0, RADIUS), h * HEAD_WIDTH : (h + 1) * HEAD_WIDTH]
            s = lax.dot_general(
                qh, keys, (((1,), (1,)), ((), ())), preferred_element_type=F32
            ) * (HEAD_WIDTH**-0.5)
            sk = sink_ref[:, h : h + 1]
            s = jnp.where(valid, s, -jnp.inf)
            top = jnp.maximum(jnp.max(s, axis=1, keepdims=True), sk)
            e = jnp.exp(s - top)
            den = jnp.sum(e, axis=1, keepdims=True) + jnp.exp(sk - top)
            p = (e * (1.0 / den)).astype(BF16)
            parts.append(jnp.dot(p, vals, preferred_element_type=F32).astype(BF16))
        return jnp.concatenate(parts, axis=1)

    attsend[...] = attend(other)
    att_copy = remote(attsend, att.at[tp], att_send_sem, att_recv_sem, partner)
    att_copy.start()
    att[tp] = attend(tp)

    for c in local_copies[:2]:
        c.wait()

    def project(p):
        w = wobuf[pl.ds(pl.multiple_of(p * width, width), width), :]
        return jnp.dot(att[p], w, preferred_element_type=F32)

    mixed[...] = resid[...].astype(F32) + project(tp)
    att_copy.wait()
    mx = mixed[...] + project(other)
    mixed[...] = mx
    scale = lax.rsqrt(jnp.mean(mx * mx, axis=1, keepdims=True) + EPS)
    normed = (mx * scale * gain_ref[...]).astype(BF16)
    spread = (picks[0] + picks[1]) if top_k == 2 else sum(picks)
    outgoing[...] = lax.dot_general(
        spread, normed, (((0,), (0,)), ((), ())), preferred_element_type=F32
    ).astype(BF16)

    def block(o):
        return pl.ds(pl.multiple_of(o * cap, cap), cap)

    def disp(o):
        return remote(
            outgoing.at[block(o)],
            landed.at[block(o)],
            d_send.at[o],
            d_recv.at[o],
            (lax.rem(sp + o, n_sp), tp),
        )

    def home(o):
        return remote(
            ret.at[block(o)],
            back.at[block(o)],
            r_send.at[o],
            r_recv.at[o],
            (lax.rem(sp + n_sp - o, n_sp), tp),
        )

    @pl.loop(1, n_sp)
    def _(o):
        disp(o).start()

    landed[0:cap, :] = outgoing[0:cap, :]

    for c in local_copies[2:]:
        c.wait()
    for c in weights:
        c.wait()

    group = max(1, min(n_sp, 128 // cap))
    grows = group * cap

    @pl.loop(0, n_sp // group)
    def _(g):
        @pl.loop(0, group)
        def _(i):
            @pl.when(g * group + i > 0)
            def _():
                disp(g * group + i).wait_recv()

        rows = pl.ds(pl.multiple_of(g * grows, grows), grows)
        x = landed[rows, :]
        acc = jnp.zeros((grows, dim), F32)
        for p in range(n_tp):
            a = jnp.dot(x, gbuf[p], preferred_element_type=F32)
            u = jnp.dot(x, ubuf[p], preferred_element_type=F32)
            hid = (a * jax.nn.sigmoid(a) * u).astype(BF16)
            part = jnp.dot(hid, dbuf[p], preferred_element_type=F32).astype(BF16)
            acc = acc + part.astype(F32)
        ret[rows, :] = acc.astype(BF16)

        @pl.loop(0, group)
        def _(i):
            @pl.when(g * group + i > 0)
            def _():
                home(g * group + i).start()

    back[0:cap, :] = ret[0:cap, :]
    w0 = rw_ref[:, 0:1]
    w1 = rw_ref[:, 1:2]
    for g in range(n_sp // group):

        @pl.loop(max(1, g * group), (g + 1) * group)
        def _(o):
            home(o).wait_recv()

        sl = slice(g * grows, (g + 1) * grows)
        chunk = back[sl, :]
        mixed[...] += w0 * jnp.dot(
            picks[0][:, sl], chunk, preferred_element_type=F32
        ) + w1 * jnp.dot(picks[1][:, sl], chunk, preferred_element_type=F32)
    out_ref[...] = mixed[...].astype(BF16)

    @pl.loop(1, n_sp)
    def _(o):
        disp(o).wait_send()
        home(o).wait_send()


def local(n_sp, n_tp, *args):
    (resid, queries, keys, values, docs, sink, w_out, gain, w_gate, w_up, w_down, ids, rw) = args
    rows_all = queries.shape[0]
    keep, dim = resid.shape
    top_k = ids.shape[1]
    cap = max(16, rows_all * top_k // n_sp)
    nb = rows_all // RADIUS
    ff = w_gate.shape[2]
    slots = n_sp * cap
    vm = pl.BlockSpec(memory_space=pltpu.VMEM)
    hbm = pl.BlockSpec(memory_space=pl.ANY)
    dma = pltpu.SemaphoreType.DMA
    return pl.pallas_call(
        functools.partial(kernel, n_sp, n_tp, cap),
        out_shape=jax.ShapeDtypeStruct((keep, dim), BF16),
        in_specs=[hbm, vm, vm, vm, vm, vm, hbm, vm, hbm, hbm, hbm, vm, vm],
        out_specs=vm,
        scratch_shapes=[
            pltpu.VMEM((rows_all + 2 * RADIUS, keys.shape[1]), BF16),
            pltpu.VMEM((rows_all + 2 * RADIUS, keys.shape[1]), BF16),
            pltpu.VMEM((nb + 2, 1, RADIUS), jnp.int32),
            pltpu.VMEM((n_tp, dim, ff), BF16),
            pltpu.VMEM((n_tp, dim, ff), BF16),
            pltpu.VMEM((n_tp, ff, dim), BF16),
            pltpu.VMEM(w_out.shape, BF16),
            pltpu.VMEM((keep, dim), BF16),
            pltpu.VMEM((n_tp, keep, queries.shape[1]), BF16),
            pltpu.VMEM((keep, queries.shape[1]), BF16),
            pltpu.VMEM((keep, dim), F32),
            pltpu.VMEM((slots, dim), BF16),
            pltpu.VMEM((slots, dim), BF16),
            pltpu.VMEM((slots, dim), BF16),
            pltpu.VMEM((slots, dim), BF16),
            dma((6,)),
            dma((6,)),
            dma((3,)),
            dma((3,)),
            dma((5,)),
            dma,
            dma,
            dma((n_sp,)),
            dma((n_sp,)),
            dma((n_sp,)),
            dma((n_sp,)),
        ],
        compiler_params=pltpu.CompilerParams(
            collective_id=0, has_side_effects=True, vmem_limit_bytes=60 * 1024 * 1024
        ),
    )(
        resid,
        queries,
        keys,
        values,
        docs.reshape(nb, 1, RADIUS),
        sink.reshape(1, -1),
        w_out,
        gain.reshape(1, -1),
        w_gate,
        w_up,
        w_down,
        ids,
        rw,
    )


def solution(mesh):
    in_specs = (
        P(("sp", "tp"), None),
        P("sp", "tp"),
        P("sp", "tp"),
        P("sp", "tp"),
        P("sp"),
        P("tp"),
        P(),
        P(),
        P("sp", None, "tp"),
        P("sp", None, "tp"),
        P("sp", "tp", None),
        P(("sp", "tp"), None),
        P(("sp", "tp"), None),
    )
    return jax.shard_map(
        functools.partial(local, mesh.shape["sp"], mesh.shape["tp"]),
        mesh=mesh,
        in_specs=in_specs,
        out_specs=P(("sp", "tp"), None),
        check_vma=False,
    )
```

```python
import functools

import jax
import jax.numpy as jnp
from jax import lax
from jax.experimental import pallas as pl
from jax.experimental.pallas import tpu as pltpu
from jax.sharding import PartitionSpec as P

HEAD_WIDTH = 128
RADIUS = 128
EPS = 1e-06
MESH = pl.DeviceIdType.MESH
F32 = jnp.float32
BF16 = jnp.bfloat16


def kernel(
    n_sp,
    n_tp,
    cap,
    parts,
    resid_hbm,
    q_ref,
    k_ref,
    v_ref,
    docs_ref,
    sink_ref,
    wout_hbm,
    gain_ref,
    gate_hbm,
    up_hbm,
    down_hbm,
    ids_ref,
    rw_ref,
    out_ref,
    kext,
    vext,
    dext,
    gbuf,
    ubuf,
    dbuf,
    wobuf,
    resid,
    att,
    attsend,
    mixed,
    outgoing,
    landed,
    ret,
    back,
    halo_send,
    halo_recv,
    w_send,
    w_recv,
    loc_sem,
    att_send_sem,
    att_recv_sem,
    d_send,
    d_recv,
    r_send,
    r_recv,
    e_send,
    e_recv,
    s_send,
    s_recv,
    x_send,
    x_recv,
    y_send,
    y_recv,
    i_send,
    i_recv,
    pids,
    prw,
    normed,
    pnormed,
    psum,
    got,
):
    sp = lax.axis_index("sp")
    tp = lax.axis_index("tp")
    other = n_tp - 1 - tp
    rows_all = q_ref.shape[0]
    heads = q_ref.shape[1] // HEAD_WIDTH
    nb = rows_all // RADIUS
    keep = rows_all // n_tp
    width = q_ref.shape[1]
    dim = out_ref.shape[1]
    total_pos = n_sp * rows_all

    barrier = pltpu.get_barrier_semaphore()

    @pl.loop(1, n_sp)
    def _(o):
        pl.semaphore_signal(
            barrier, inc=1, device_id=(lax.rem(sp + o, n_sp), tp), device_id_type=MESH
        )

    pl.semaphore_signal(barrier, inc=1, device_id=(sp, other), device_id_type=MESH)

    local_copies = [
        pltpu.make_async_copy(wout_hbm, wobuf, loc_sem.at[0]),
        pltpu.make_async_copy(resid_hbm, resid, loc_sem.at[1]),
        pltpu.make_async_copy(gate_hbm.at[0], gbuf.at[tp], loc_sem.at[2]),
        pltpu.make_async_copy(up_hbm.at[0], ubuf.at[tp], loc_sem.at[3]),
        pltpu.make_async_copy(down_hbm.at[0], dbuf.at[tp], loc_sem.at[4]),
    ]
    for c in local_copies[:2]:
        c.start()

    pl.semaphore_wait(barrier, n_sp)

    right = (lax.rem(sp + 1, n_sp), tp)
    left = (lax.rem(sp + n_sp - 1, n_sp), tp)
    tail = rows_all - RADIUS
    end = rows_all + RADIUS

    def remote(src, dst, s, r, dev):
        return pltpu.make_async_remote_copy(
            src_ref=src, dst_ref=dst, send_sem=s, recv_sem=r, device_id=dev, device_id_type=MESH
        )

    halo = []
    for i, (src, dst) in enumerate(((k_ref, kext), (v_ref, vext))):
        halo.append(
            remote(
                src.at[pl.ds(tail, RADIUS)],
                dst.at[pl.ds(0, RADIUS)],
                halo_send.at[2 * i],
                halo_recv.at[2 * i],
                right,
            )
        )
        halo.append(
            remote(
                src.at[pl.ds(0, RADIUS)],
                dst.at[pl.ds(end, RADIUS)],
                halo_send.at[2 * i + 1],
                halo_recv.at[2 * i + 1],
                left,
            )
        )
    halo.append(
        remote(docs_ref.at[nb - 1], dext.at[0], halo_send.at[4], halo_recv.at[4], right)
    )
    halo.append(
        remote(docs_ref.at[0], dext.at[nb + 1], halo_send.at[5], halo_recv.at[5], left)
    )
    for c in halo:
        c.start()
    partner = (sp, other)
    peer = (lax.rem(sp + n_sp // 2, n_sp), tp)
    small = [
        remote(ids_ref, pids, i_send.at[0], i_recv.at[0], peer),
        remote(rw_ref, prw, i_send.at[1], i_recv.at[1], peer),
    ]
    for c in small:
        c.start()
    weights = [
        remote(gate_hbm.at[0], gbuf.at[tp], w_send.at[0], w_recv.at[0], partner),
        remote(up_hbm.at[0], ubuf.at[tp], w_send.at[1], w_recv.at[1], partner),
        remote(down_hbm.at[0], dbuf.at[tp], w_send.at[2], w_recv.at[2], partner),
    ]
    for c in weights:
        c.start()
    for c in local_copies[2:]:
        c.start()

    kext[RADIUS:end, :] = k_ref[...]
    vext[RADIUS:end, :] = v_ref[...]
    for b in range(nb):
        dext[b + 1] = docs_ref[b]

    half = n_sp // 2
    base = (sp // half) * half
    mine = lax.rem(sp, half)
    top_k = ids_ref.shape[1]
    n_slots = half * cap
    lane = lax.broadcasted_iota(jnp.int32, (keep, n_sp), 1)
    lower = (
        lax.broadcasted_iota(jnp.int32, (keep, keep), 1)
        < lax.broadcasted_iota(jnp.int32, (keep, keep), 0)
    ).astype(BF16)
    slot_lane = lax.broadcasted_iota(jnp.int32, (keep, n_slots), 1).astype(F32)

    def route(ref):
        hots = [(ref[:, k : k + 1] == lane).astype(F32) for k in range(top_k)]
        before = jnp.dot(lower, sum(hots).astype(BF16), preferred_element_type=F32)
        picks = []
        for k in range(top_k):
            rank = jnp.sum(hots[k] * before, axis=1, keepdims=True)
            at = ref[:, k : k + 1] - base
            here = (at >= 0) & (at < half)
            rel = at - mine
            rel = jnp.where(rel < 0, rel + half, rel)
            slot = jnp.where(here, rel.astype(F32) * float(cap) + rank, -1.0)
            picks.append((slot == slot_lane).astype(BF16))
        return picks

    picks = route(ids_ref)

    for c in halo:
        c.wait()

    eye = lax.broadcasted_iota(jnp.int32, (RADIUS, RADIUS), 0) == lax.broadcasted_iota(
        jnp.int32, (RADIUS, RADIUS), 1
    )

    def attend(b):
        row0 = pl.multiple_of(b * RADIUS, RADIUS)
        keys = kext[pl.ds(row0, 3 * RADIUS), :]
        vals = vext[pl.ds(row0, 3 * RADIUS), :]
        kdoc = jnp.concatenate([dext[b], dext[b + 1], dext[b + 2]], axis=1)
        qdoc = jnp.sum(
            jnp.where(eye, jnp.broadcast_to(dext[b + 1], (RADIUS, RADIUS)), 0).astype(F32),
            axis=1,
            keepdims=True,
        )
        qi = lax.broadcasted_iota(jnp.int32, (RADIUS, 3 * RADIUS), 0)
        kj = lax.broadcasted_iota(jnp.int32, (RADIUS, 3 * RADIUS), 1)
        where_key = kj + (sp * rows_all + (b - 1) * RADIUS)
        valid = (
            (kj >= qi)
            & (kj <= qi + 2 * RADIUS)
            & (where_key >= 0)
            & (where_key < total_pos)
            & (kdoc.astype(F32) == qdoc)
        )
        parts = []
        for h in range(heads):
            qh = q_ref[pl.ds(row0, RADIUS), h * HEAD_WIDTH : (h + 1) * HEAD_WIDTH]
            s = lax.dot_general(
                qh, keys, (((1,), (1,)), ((), ())), preferred_element_type=F32
            ) * (HEAD_WIDTH**-0.5)
            sk = sink_ref[:, h : h + 1]
            s = jnp.where(valid, s, -jnp.inf)
            top = jnp.maximum(jnp.max(s, axis=1, keepdims=True), sk)
            e = jnp.exp(s - top)
            den = jnp.sum(e, axis=1, keepdims=True) + jnp.exp(sk - top)
            p = (e * (1.0 / den)).astype(BF16)
            parts.append(jnp.dot(p, vals, preferred_element_type=F32).astype(BF16))
        return jnp.concatenate(parts, axis=1)

    attsend[...] = attend(other)
    att_copy = remote(attsend, att.at[tp], att_send_sem, att_recv_sem, partner)
    att_copy.start()
    att[tp] = attend(tp)

    for c in local_copies[:2]:
        c.wait()

    def project(p):
        w = wobuf[pl.ds(pl.multiple_of(p * width, width), width), :]
        return jnp.dot(att[p], w, preferred_element_type=F32)

    mixed[...] = resid[...].astype(F32) + project(tp)
    att_copy.wait()
    mx = mixed[...] + project(other)
    mixed[...] = mx
    scale = lax.rsqrt(jnp.mean(mx * mx, axis=1, keepdims=True) + EPS)
    normed[...] = (mx * scale * gain_ref[...]).astype(BF16)
    wide = dim // parts

    def cols(c):
        return pl.ds(c * wide, wide)

    swaps = [
        remote(
            normed.at[:, cols(c)], pnormed.at[:, cols(c)], x_send.at[c], x_recv.at[c], peer
        )
        for c in range(parts)
    ]
    for c in swaps:
        c.start()

    def spread(chosen, rows):
        return lax.dot_general(
            sum(chosen), rows, (((0,), (0,)), ((), ())), preferred_element_type=F32
        ).astype(BF16)

    def block(o, first=0):
        return pl.ds(pl.multiple_of(first + o * cap, cap), cap)

    def to(o):
        return (base + lax.rem(mine + o, half), tp)

    def fro(o):
        return (base + lax.rem(mine + half - o, half), tp)

    def disp(o):
        return remote(
            outgoing.at[block(o)], landed.at[block(o)], d_send.at[o], d_recv.at[o], to(o)
        )

    def home(o):
        return remote(ret.at[block(o)], back.at[block(o)], r_send.at[o], r_recv.at[o], fro(o))

    def disp2(o, c):
        sl = (block(o, n_slots), cols(c))
        i = c * half + o
        return remote(outgoing.at[sl], landed.at[sl], e_send.at[i], e_recv.at[i], to(o))

    def home2(o, c):
        sl = (block(o, n_slots), cols(c))
        i = c * half + o
        return remote(ret.at[sl], back.at[sl], s_send.at[i], s_recv.at[i], fro(o))

    outgoing[0:n_slots, :] = spread(picks, normed[...])

    @pl.loop(1, half)
    def _(o):
        disp(o).start()

    landed[0:cap, :] = outgoing[0:cap, :]

    for c in small:
        c.wait()
    ppicks = route(pids)
    for c in range(parts):
        swaps[c].wait_recv()
        cs = slice(c * wide, (c + 1) * wide)
        outgoing[n_slots : 2 * n_slots, cs] = spread(ppicks, pnormed[:, cs])

        @pl.loop(1, half)
        def _(o):
            disp2(o, c).start()

    landed[n_slots : n_slots + cap, :] = outgoing[n_slots : n_slots + cap, :]

    for c in local_copies[2:]:
        c.wait()
    for c in weights:
        c.wait()

    def experts(rows, count):
        x = landed[rows, :]
        acc = jnp.zeros((count, dim), F32)
        for p in range(n_tp):
            a = jnp.dot(x, gbuf[p], preferred_element_type=F32)
            u = jnp.dot(x, ubuf[p], preferred_element_type=F32)
            hid = (a * jax.nn.sigmoid(a) * u).astype(BF16)
            part = jnp.dot(hid, dbuf[p], preferred_element_type=F32).astype(BF16)
            acc = acc + part.astype(F32)
        ret[rows, :] = acc.astype(BF16)

    @pl.loop(1, half)
    def _(o):
        disp(o).wait_recv()

    experts(slice(0, n_slots), n_slots)

    @pl.loop(1, half)
    def _(o):
        home(o).start()

    back[0:cap, :] = ret[0:cap, :]

    group = max(1, min(half, 128 // cap))
    grows = group * cap

    @pl.loop(0, half // group)
    def _(g):
        @pl.loop(0, group)
        def _(i):
            @pl.when(g * group + i > 0)
            def _():
                for c in range(parts):
                    disp2(g * group + i, c).wait_recv()

        experts(pl.ds(pl.multiple_of(n_slots + g * grows, grows), grows), grows)

        for c in range(parts):

            @pl.loop(0, group)
            def _(i):
                @pl.when(g * group + i > 0)
                def _():
                    home2(g * group + i, c).start()

    back[n_slots : n_slots + cap, :] = ret[n_slots : n_slots + cap, :]

    def gathered(chosen, weight_ref, first, cs):
        chunk = back[first : first + n_slots, cs]
        return sum(
            weight_ref[:, k : k + 1] * jnp.dot(chosen[k], chunk, preferred_element_type=F32)
            for k in range(top_k)
        )

    crossings = [
        remote(psum.at[:, cols(c)], got.at[:, cols(c)], y_send.at[c], y_recv.at[c], peer)
        for c in range(parts)
    ]
    for c in range(parts):

        @pl.loop(1, half)
        def _(o):
            home2(o, c).wait_recv()

        cs = slice(c * wide, (c + 1) * wide)
        psum[:, cs] = gathered(ppicks, prw, n_slots, cs).astype(BF16)
        crossings[c].start()

    @pl.loop(1, half)
    def _(o):
        home(o).wait_recv()

    mixed[...] += gathered(picks, rw_ref, 0, slice(0, dim))
    for c in range(parts):
        crossings[c].wait_recv()
        cs = slice(c * wide, (c + 1) * wide)
        out_ref[:, cs] = (mixed[:, cs] + got[:, cs].astype(F32)).astype(BF16)

    for c in range(parts):
        swaps[c].wait_send()
        crossings[c].wait_send()

    @pl.loop(1, half)
    def _(o):
        disp(o).wait_send()
        home(o).wait_send()
        for c in range(parts):
            disp2(o, c).wait_send()
            home2(o, c).wait_send()


def local(n_sp, n_tp, *args):
    (resid, queries, keys, values, docs, sink, w_out, gain, w_gate, w_up, w_down, ids, rw) = args
    rows_all = queries.shape[0]
    keep, dim = resid.shape
    top_k = ids.shape[1]
    cap = max(16, rows_all * top_k // n_sp)
    nb = rows_all // RADIUS
    parts = 2
    half = n_sp // 2
    ff = w_gate.shape[2]
    slots = n_sp * cap
    vm = pl.BlockSpec(memory_space=pltpu.VMEM)
    hbm = pl.BlockSpec(memory_space=pl.ANY)
    dma = pltpu.SemaphoreType.DMA
    return pl.pallas_call(
        functools.partial(kernel, n_sp, n_tp, cap, parts),
        out_shape=jax.ShapeDtypeStruct((keep, dim), BF16),
        in_specs=[hbm, vm, vm, vm, vm, vm, hbm, vm, hbm, hbm, hbm, vm, vm],
        out_specs=vm,
        scratch_shapes=[
            pltpu.VMEM((rows_all + 2 * RADIUS, keys.shape[1]), BF16),
            pltpu.VMEM((rows_all + 2 * RADIUS, keys.shape[1]), BF16),
            pltpu.VMEM((nb + 2, 1, RADIUS), jnp.int32),
            pltpu.VMEM((n_tp, dim, ff), BF16),
            pltpu.VMEM((n_tp, dim, ff), BF16),
            pltpu.VMEM((n_tp, ff, dim), BF16),
            pltpu.VMEM(w_out.shape, BF16),
            pltpu.VMEM((keep, dim), BF16),
            pltpu.VMEM((n_tp, keep, queries.shape[1]), BF16),
            pltpu.VMEM((keep, queries.shape[1]), BF16),
            pltpu.VMEM((keep, dim), F32),
            pltpu.VMEM((slots, dim), BF16),
            pltpu.VMEM((slots, dim), BF16),
            pltpu.VMEM((slots, dim), BF16),
            pltpu.VMEM((slots, dim), BF16),
            dma((6,)),
            dma((6,)),
            dma((3,)),
            dma((3,)),
            dma((5,)),
            dma,
            dma,
            dma((half,)),
            dma((half,)),
            dma((half,)),
            dma((half,)),
            dma((parts * half,)),
            dma((parts * half,)),
            dma((parts * half,)),
            dma((parts * half,)),
            dma((parts,)),
            dma((parts,)),
            dma((parts,)),
            dma((parts,)),
            dma((2,)),
            dma((2,)),
            pltpu.VMEM(ids.shape, jnp.int32),
            pltpu.VMEM(rw.shape, F32),
            pltpu.VMEM((keep, dim), BF16),
            pltpu.VMEM((keep, dim), BF16),
            pltpu.VMEM((keep, dim), BF16),
            pltpu.VMEM((keep, dim), BF16),
        ],
        compiler_params=pltpu.CompilerParams(
            collective_id=0, has_side_effects=True, vmem_limit_bytes=60 * 1024 * 1024
        ),
    )(
        resid,
        queries,
        keys,
        values,
        docs.reshape(nb, 1, RADIUS),
        sink.reshape(1, -1),
        w_out,
        gain.reshape(1, -1),
        w_gate,
        w_up,
        w_down,
        ids,
        rw,
    )


def solution(mesh):
    in_specs = (
        P(("sp", "tp"), None),
        P("sp", "tp"),
        P("sp", "tp"),
        P("sp", "tp"),
        P("sp"),
        P("tp"),
        P(),
        P(),
        P("sp", None, "tp"),
        P("sp", None, "tp"),
        P("sp", "tp", None),
        P(("sp", "tp"), None),
        P(("sp", "tp"), None),
    )
    return jax.shard_map(
        functools.partial(local, mesh.shape["sp"], mesh.shape["tp"]),
        mesh=mesh,
        in_specs=in_specs,
        out_specs=P(("sp", "tp"), None),
        check_vma=False,
    )
```

```python
import functools

import jax
import jax.numpy as jnp
from jax import lax
from jax.experimental import pallas as pl
from jax.experimental.pallas import tpu as pltpu
from jax.sharding import PartitionSpec as P

HEAD_WIDTH = 128
RADIUS = 128
EPS = 1e-06
MESH = pl.DeviceIdType.MESH
F32 = jnp.float32
BF16 = jnp.bfloat16


def kernel(
    n_sp,
    n_tp,
    cap,
    parts,
    resid_hbm,
    q_ref,
    k_ref,
    v_ref,
    docs_ref,
    sink_ref,
    wout_hbm,
    gain_ref,
    gate_hbm,
    up_hbm,
    down_hbm,
    ids_ref,
    rw_ref,
    out_ref,
    kext,
    vext,
    dext,
    gbuf,
    ubuf,
    dbuf,
    wobuf,
    resid,
    att,
    attsend,
    mixed,
    outgoing,
    landed,
    ret,
    back,
    halo_send,
    halo_recv,
    w_send,
    w_recv,
    loc_sem,
    att_send_sem,
    att_recv_sem,
    d_send,
    d_recv,
    r_send,
    r_recv,
    e_send,
    e_recv,
    s_send,
    s_recv,
    x_send,
    x_recv,
    y_send,
    y_recv,
    i_send,
    i_recv,
    pids,
    prw,
    normed,
    pnormed,
    psum,
    got,
):
    sp = lax.axis_index("sp")
    tp = lax.axis_index("tp")
    other = n_tp - 1 - tp
    rows_all = q_ref.shape[0]
    heads = q_ref.shape[1] // HEAD_WIDTH
    nb = rows_all // RADIUS
    keep = rows_all // n_tp
    width = q_ref.shape[1]
    dim = out_ref.shape[1]
    total_pos = n_sp * rows_all

    barrier = pltpu.get_barrier_semaphore()

    half = n_sp // 2
    base = (sp // half) * half
    mine = lax.rem(sp, half)
    partner = (sp, other)
    peer = (lax.rem(sp + half, n_sp), tp)
    right = (lax.rem(sp + 1, n_sp), tp)
    left = (lax.rem(sp + n_sp - 1, n_sp), tp)

    def hello(dev):
        pl.semaphore_signal(barrier, inc=1, device_id=dev, device_id_type=MESH)

    def if_left(f):
        pl.when(sp > 0)(f)

    def if_right(f):
        pl.when(sp < n_sp - 1)(f)

    hello(peer)
    if_left(lambda: hello(left))
    if_right(lambda: hello(right))
    hello(partner)

    @pl.loop(1, half)
    def _(o):
        hello((base + lax.rem(mine + o, half), tp))

    local_copies = [
        pltpu.make_async_copy(wout_hbm, wobuf, loc_sem.at[0]),
        pltpu.make_async_copy(resid_hbm, resid, loc_sem.at[1]),
        pltpu.make_async_copy(gate_hbm.at[0], gbuf.at[tp], loc_sem.at[2]),
        pltpu.make_async_copy(up_hbm.at[0], ubuf.at[tp], loc_sem.at[3]),
        pltpu.make_async_copy(down_hbm.at[0], dbuf.at[tp], loc_sem.at[4]),
    ]
    for c in local_copies[:2]:
        c.start()

    tail = rows_all - RADIUS
    end = rows_all + RADIUS
    kext[RADIUS:end, :] = k_ref[...]
    vext[RADIUS:end, :] = v_ref[...]
    for b in range(nb):
        dext[b + 1] = docs_ref[b]

    def blank(row, b):
        def fill():
            zero = jnp.zeros((RADIUS, kext.shape[1]), BF16)
            kext[row : row + RADIUS, :] = zero
            vext[row : row + RADIUS, :] = zero
            dext[b] = jnp.zeros((1, RADIUS), jnp.int32)

        return fill

    pl.when(sp == 0)(blank(0, 0))
    pl.when(sp == n_sp - 1)(blank(end, nb + 1))

    has_left = (sp + n_sp - 1) // n_sp
    has_right = (2 * n_sp - 2 - sp) // n_sp
    pl.semaphore_wait(barrier, half + 1 + has_left + has_right)

    def remote(src, dst, s, r, dev):
        return pltpu.make_async_remote_copy(
            src_ref=src, dst_ref=dst, send_sem=s, recv_sem=r, device_id=dev, device_id_type=MESH
        )

    halo = []
    for i, (src, dst) in enumerate(((k_ref, kext), (v_ref, vext))):
        halo.append(
            remote(
                src.at[pl.ds(tail, RADIUS)],
                dst.at[pl.ds(0, RADIUS)],
                halo_send.at[2 * i],
                halo_recv.at[2 * i],
                right,
            )
        )
        halo.append(
            remote(
                src.at[pl.ds(0, RADIUS)],
                dst.at[pl.ds(end, RADIUS)],
                halo_send.at[2 * i + 1],
                halo_recv.at[2 * i + 1],
                left,
            )
        )
    halo.append(
        remote(docs_ref.at[nb - 1], dext.at[0], halo_send.at[4], halo_recv.at[4], right)
    )
    halo.append(
        remote(docs_ref.at[0], dext.at[nb + 1], halo_send.at[5], halo_recv.at[5], left)
    )
    for i in range(0, len(halo), 2):
        if_right(halo[i].start)
        if_left(halo[i + 1].start)
    small = [
        remote(ids_ref, pids, i_send.at[0], i_recv.at[0], peer),
        remote(rw_ref, prw, i_send.at[1], i_recv.at[1], peer),
    ]
    for c in small:
        c.start()
    weights = [
        remote(gate_hbm.at[0], gbuf.at[tp], w_send.at[0], w_recv.at[0], partner),
        remote(up_hbm.at[0], ubuf.at[tp], w_send.at[1], w_recv.at[1], partner),
        remote(down_hbm.at[0], dbuf.at[tp], w_send.at[2], w_recv.at[2], partner),
    ]

    top_k = ids_ref.shape[0]
    n_slots = half * cap
    lane = lax.broadcasted_iota(jnp.int32, (keep, n_sp), 1).astype(F32)
    base_f = base.astype(F32)
    mine_f = mine.astype(F32)
    lower = (
        lax.broadcasted_iota(jnp.int32, (keep, keep), 1)
        < lax.broadcasted_iota(jnp.int32, (keep, keep), 0)
    ).astype(BF16)
    slot_lane = lax.broadcasted_iota(jnp.int32, (keep, n_slots), 1).astype(F32)

    square = lax.broadcasted_iota(jnp.int32, (keep, keep), 0) == lax.broadcasted_iota(
        jnp.int32, (keep, keep), 1
    )

    def column(ref, k):
        row = jnp.broadcast_to(ref[k : k + 1, :].astype(F32), (keep, keep))
        return jnp.sum(jnp.where(square, row, 0.0), axis=1, keepdims=True)

    def route(ref):
        ids = [column(ref, k) for k in range(top_k)]
        hots = [(e == lane).astype(F32) for e in ids]
        before = jnp.dot(lower, sum(hots).astype(BF16), preferred_element_type=F32)
        picks = []
        for k in range(top_k):
            rank = jnp.sum(hots[k] * before, axis=1, keepdims=True)
            at = ids[k] - base_f
            here = (at >= 0) & (at < half)
            rel = at - mine_f
            rel = jnp.where(rel < 0, rel + half, rel)
            slot = jnp.where(here, rel * float(cap) + rank, -1.0)
            picks.append((slot == slot_lane).astype(BF16))
        return picks

    picks = route(ids_ref)

    for i in range(0, len(halo), 2):
        if_left(halo[i].wait_recv)
        if_right(halo[i + 1].wait_recv)

    eye = lax.broadcasted_iota(jnp.int32, (RADIUS, RADIUS), 0) == lax.broadcasted_iota(
        jnp.int32, (RADIUS, RADIUS), 1
    )

    def attend(b):
        row0 = pl.multiple_of(b * RADIUS, RADIUS)
        keys = kext[pl.ds(row0, 3 * RADIUS), :]
        vals = vext[pl.ds(row0, 3 * RADIUS), :]
        kdoc = jnp.concatenate([dext[b], dext[b + 1], dext[b + 2]], axis=1)
        qdoc = jnp.sum(
            jnp.where(eye, jnp.broadcast_to(dext[b + 1], (RADIUS, RADIUS)), 0).astype(F32),
            axis=1,
            keepdims=True,
        )
        qi = lax.broadcasted_iota(jnp.int32, (RADIUS, 3 * RADIUS), 0)
        kj = lax.broadcasted_iota(jnp.int32, (RADIUS, 3 * RADIUS), 1)
        where_key = kj + (sp * rows_all + (b - 1) * RADIUS)
        valid = (
            (kj >= qi)
            & (kj <= qi + 2 * RADIUS)
            & (where_key >= 0)
            & (where_key < total_pos)
            & (kdoc.astype(F32) == qdoc)
        )
        parts = []
        for h in range(heads):
            qh = q_ref[pl.ds(row0, RADIUS), h * HEAD_WIDTH : (h + 1) * HEAD_WIDTH]
            s = lax.dot_general(
                qh, keys, (((1,), (1,)), ((), ())), preferred_element_type=F32
            ) * (HEAD_WIDTH**-0.5)
            sk = sink_ref[:, h : h + 1]
            s = jnp.where(valid, s, -jnp.inf)
            top = jnp.maximum(jnp.max(s, axis=1, keepdims=True), sk)
            e = jnp.exp(s - top)
            den = jnp.sum(e, axis=1, keepdims=True) + jnp.exp(sk - top)
            p = (e * (1.0 / den)).astype(BF16)
            parts.append(jnp.dot(p, vals, preferred_element_type=F32).astype(BF16))
        return jnp.concatenate(parts, axis=1)

    attsend[...] = attend(other)
    att_copy = remote(attsend, att.at[tp], att_send_sem, att_recv_sem, partner)
    att_copy.start()
    for c in weights:
        c.start()
    for c in local_copies[2:]:
        c.start()
    att[tp] = attend(tp)

    for c in local_copies[:2]:
        c.wait()

    def project(p):
        w = wobuf[pl.ds(pl.multiple_of(p * width, width), width), :]
        return jnp.dot(att[p], w, preferred_element_type=F32)

    mixed[...] = resid[...].astype(F32) + project(tp)
    att_copy.wait()
    mx = mixed[...] + project(other)
    mixed[...] = mx
    scale = lax.rsqrt(jnp.mean(mx * mx, axis=1, keepdims=True) + EPS)
    normed[...] = (mx * scale * gain_ref[...]).astype(BF16)
    wide = dim // parts

    def cols(c):
        return pl.ds(c * wide, wide)

    swaps = [
        remote(
            normed.at[:, cols(c)], pnormed.at[:, cols(c)], x_send.at[c], x_recv.at[c], peer
        )
        for c in range(parts)
    ]
    for c in swaps:
        c.start()

    def spread(chosen, rows):
        return lax.dot_general(
            sum(chosen), rows, (((0,), (0,)), ((), ())), preferred_element_type=F32
        ).astype(BF16)

    def block(o, first=0):
        return pl.ds(pl.multiple_of(first + o * cap, cap), cap)

    def to(o):
        return (base + lax.rem(mine + o, half), tp)

    def fro(o):
        return (base + lax.rem(mine + half - o, half), tp)

    def disp(o):
        return remote(
            outgoing.at[block(o)], landed.at[block(o)], d_send.at[o], d_recv.at[o], to(o)
        )

    def home(o):
        return remote(ret.at[block(o)], back.at[block(o)], r_send.at[o], r_recv.at[o], fro(o))

    def disp2(o, c):
        sl = (block(o, n_slots), cols(c))
        i = c * half + o
        return remote(outgoing.at[sl], landed.at[sl], e_send.at[i], e_recv.at[i], to(o))

    def home2(o, c):
        sl = (block(o, n_slots), cols(c))
        i = c * half + o
        return remote(ret.at[sl], back.at[sl], s_send.at[i], s_recv.at[i], fro(o))

    outgoing[0:n_slots, :] = spread(picks, normed[...])

    @pl.loop(1, half)
    def _(o):
        disp(o).start()

    landed[0:cap, :] = outgoing[0:cap, :]

    for c in small:
        c.wait()
    ppicks = route(pids)
    for c in range(parts):
        swaps[c].wait_recv()
        cs = slice(c * wide, (c + 1) * wide)
        outgoing[n_slots : 2 * n_slots, cs] = spread(ppicks, pnormed[:, cs])

        @pl.loop(1, half)
        def _(o):
            disp2(o, c).start()

    landed[n_slots : n_slots + cap, :] = outgoing[n_slots : n_slots + cap, :]

    for c in local_copies[2:]:
        c.wait()
    for c in weights:
        c.wait()

    def experts(rows, count):
        x = landed[rows, :]
        acc = jnp.zeros((count, dim), F32)
        for p in range(n_tp):
            a = jnp.dot(x, gbuf[p], preferred_element_type=F32)
            u = jnp.dot(x, ubuf[p], preferred_element_type=F32)
            hid = (a * jax.nn.sigmoid(a) * u).astype(BF16)
            part = jnp.dot(hid, dbuf[p], preferred_element_type=F32).astype(BF16)
            acc = acc + part.astype(F32)
        ret[rows, :] = acc.astype(BF16)

    @pl.loop(1, half)
    def _(o):
        disp(o).wait_recv()

    experts(slice(0, n_slots), n_slots)

    back[0:cap, :] = ret[0:cap, :]

    group = max(1, min(half, 128 // cap))
    grows = group * cap

    @pl.loop(0, half // group)
    def _(g):
        @pl.loop(0, group)
        def _(i):
            @pl.when(g * group + i > 0)
            def _():
                for c in range(parts):
                    disp2(g * group + i, c).wait_recv()

        experts(pl.ds(pl.multiple_of(n_slots + g * grows, grows), grows), grows)

        for c in range(parts):

            @pl.loop(0, group)
            def _(i):
                @pl.when(g * group + i > 0)
                def _():
                    home2(g * group + i, c).start()

    @pl.loop(1, half)
    def _(o):
        home(o).start()

    back[n_slots : n_slots + cap, :] = ret[n_slots : n_slots + cap, :]

    def gathered(chosen, weight_ref, first, cs):
        chunk = back[first : first + n_slots, cs]
        return sum(
            column(weight_ref, k) * jnp.dot(chosen[k], chunk, preferred_element_type=F32)
            for k in range(top_k)
        )

    crossings = [
        remote(psum.at[:, cols(c)], got.at[:, cols(c)], y_send.at[c], y_recv.at[c], peer)
        for c in range(parts)
    ]
    for c in range(parts):

        @pl.loop(1, half)
        def _(o):
            home2(o, c).wait_recv()

        cs = slice(c * wide, (c + 1) * wide)
        psum[:, cs] = gathered(ppicks, prw, n_slots, cs).astype(BF16)
        crossings[c].start()

    @pl.loop(1, half)
    def _(o):
        home(o).wait_recv()

    mixed[...] += gathered(picks, rw_ref, 0, slice(0, dim))
    for c in range(parts):
        crossings[c].wait_recv()
        cs = slice(c * wide, (c + 1) * wide)
        out_ref[:, cs] = (mixed[:, cs] + got[:, cs].astype(F32)).astype(BF16)

    for i in range(0, len(halo), 2):
        if_right(halo[i].wait_send)
        if_left(halo[i + 1].wait_send)
    for c in range(parts):
        swaps[c].wait_send()
        crossings[c].wait_send()

    @pl.loop(1, half)
    def _(o):
        disp(o).wait_send()
        home(o).wait_send()
        for c in range(parts):
            disp2(o, c).wait_send()
            home2(o, c).wait_send()


def local(n_sp, n_tp, *args):
    (resid, queries, keys, values, docs, sink, w_out, gain, w_gate, w_up, w_down, ids, rw) = args
    rows_all = queries.shape[0]
    keep, dim = resid.shape
    top_k = ids.shape[1]
    cap = max(16, rows_all * top_k // n_sp)
    nb = rows_all // RADIUS
    parts = 2
    half = n_sp // 2
    ff = w_gate.shape[2]
    slots = n_sp * cap
    vm = pl.BlockSpec(memory_space=pltpu.VMEM)
    hbm = pl.BlockSpec(memory_space=pl.ANY)
    dma = pltpu.SemaphoreType.DMA
    return pl.pallas_call(
        functools.partial(kernel, n_sp, n_tp, cap, parts),
        out_shape=jax.ShapeDtypeStruct((keep, dim), BF16),
        in_specs=[hbm, vm, vm, vm, vm, vm, hbm, vm, hbm, hbm, hbm, vm, vm],
        out_specs=vm,
        scratch_shapes=[
            pltpu.VMEM((rows_all + 2 * RADIUS, keys.shape[1]), BF16),
            pltpu.VMEM((rows_all + 2 * RADIUS, keys.shape[1]), BF16),
            pltpu.VMEM((nb + 2, 1, RADIUS), jnp.int32),
            pltpu.VMEM((n_tp, dim, ff), BF16),
            pltpu.VMEM((n_tp, dim, ff), BF16),
            pltpu.VMEM((n_tp, ff, dim), BF16),
            pltpu.VMEM(w_out.shape, BF16),
            pltpu.VMEM((keep, dim), BF16),
            pltpu.VMEM((n_tp, keep, queries.shape[1]), BF16),
            pltpu.VMEM((keep, queries.shape[1]), BF16),
            pltpu.VMEM((keep, dim), F32),
            pltpu.VMEM((slots, dim), BF16),
            pltpu.VMEM((slots, dim), BF16),
            pltpu.VMEM((slots, dim), BF16),
            pltpu.VMEM((slots, dim), BF16),
            dma((6,)),
            dma((6,)),
            dma((3,)),
            dma((3,)),
            dma((5,)),
            dma,
            dma,
            dma((half,)),
            dma((half,)),
            dma((half,)),
            dma((half,)),
            dma((parts * half,)),
            dma((parts * half,)),
            dma((parts * half,)),
            dma((parts * half,)),
            dma((parts,)),
            dma((parts,)),
            dma((parts,)),
            dma((parts,)),
            dma((2,)),
            dma((2,)),
            pltpu.VMEM(ids.shape[::-1], jnp.int32),
            pltpu.VMEM(rw.shape[::-1], F32),
            pltpu.VMEM((keep, dim), BF16),
            pltpu.VMEM((keep, dim), BF16),
            pltpu.VMEM((keep, dim), BF16),
            pltpu.VMEM((keep, dim), BF16),
        ],
        compiler_params=pltpu.CompilerParams(
            collective_id=0, has_side_effects=True, vmem_limit_bytes=60 * 1024 * 1024
        ),
    )(
        resid,
        queries,
        keys,
        values,
        docs.reshape(nb, 1, RADIUS),
        sink.reshape(1, -1),
        w_out,
        gain.reshape(1, -1),
        w_gate,
        w_up,
        w_down,
        ids.T,
        rw.T,
    )


def solution(mesh):
    in_specs = (
        P(("sp", "tp"), None),
        P("sp", "tp"),
        P("sp", "tp"),
        P("sp", "tp"),
        P("sp"),
        P("tp"),
        P(),
        P(),
        P("sp", None, "tp"),
        P("sp", None, "tp"),
        P("sp", "tp", None),
        P(("sp", "tp"), None),
        P(("sp", "tp"), None),
    )
    return jax.shard_map(
        functools.partial(local, mesh.shape["sp"], mesh.shape["tp"]),
        mesh=mesh,
        in_specs=in_specs,
        out_specs=P(("sp", "tp"), None),
        check_vma=False,
    )
```
